32 devices in a mesh: sp: 16 (over z, y, x), tp: 2 (over core).
Axes of the slice: x: 2, y: 2, z: 4, core: 2. Of those that a mesh axis runs over, the one named last changes fastest.
Arguments:
- tokens: bfloat16 [4096, 2048], P('sp', 'tp'), may hold values from -6 to 6
- norm_gain: float32 [2048], replicated, may hold values from 0.1 to 1.9
- query_one: bfloat16 [2048, 512], P(None, 'tp'), may hold values from -6 to 6
- key_one: bfloat16 [2048, 512], P(None, 'tp'), may hold values from -1 to 1
- query_two: bfloat16 [2048, 512], P(None, 'tp'), may hold values from -6 to 6
- key_two: bfloat16 [2048, 512], P(None, 'tp'), may hold values from -1 to 1
- value_weight: bfloat16 [2048, 1024], P(None, 'tp'), may hold values from -0.125 to 0.125
- attn_gate_weight: bfloat16 [2048, 1024], P(None, 'tp'), may hold values from -0.125 to 0.125
- conv_outer: bfloat16 [2048, 1024], P(None, 'tp'), may hold values from -0.125 to 0.125
- conv_inner: bfloat16 [2048, 1024], P(None, 'tp'), may hold values from -0.125 to 0.125
- conv_input: bfloat16 [2048, 1024], P(None, 'tp'), may hold values from -0.125 to 0.125
- conv_taps: bfloat16 [3, 1024], P(None, 'tp'), may hold values from -3.5 to 3.5
- head_lambda: float32 [8], P('tp'), may hold values from 0.3 to 0.8
- head_gain: float32 [128], replicated, may hold values from 0.1 to 1.9
- attn_out_weight: bfloat16 [1024, 2048], P('tp'), may hold values from -0.125 to 0.125
- conv_out_weight: bfloat16 [1024, 2048], P('tp'), may hold values from -0.125 to 0.125
Outputs:
- mixed: bfloat16 [4096, 2048], P(('sp', 'tp'))
The draws below stay inside these ranges and needn't reach their ends.
All inputs are finite; a program needn't handle non-finite values.
Results may differ from the reference program's by a relative error of at most 0.014.
Values may be sent and summed in bfloat16 or wider, within the bound.
A program may use at most 128 MiB of HBM per device.

```python
import math
import jax
import jax.numpy as jnp
from jax import lax

D = 2048
HEADS = 8
KEY_DIM = 64
VALUE_DIM = 128
CONV_CH = 1024
TOKENS = 4096
N_TP = 2


def draw_tokens(key, part):
    drawn = jax.random.normal(jax.random.fold_in(key, 102), (TOKENS, D), jnp.float32)
    return jnp.clip(drawn, -6.0, 6.0).astype(jnp.bfloat16)


def pair_draw(key, index):
    base = jax.random.fold_in(key, index)
    key_part, other_part = jax.random.split(base, 2)
    shape = (D, HEADS * KEY_DIM)
    factor = 1.0 / math.sqrt(D)
    key_matrix = jnp.clip(jax.random.normal(key_part, shape, jnp.float32), -6.0, 6.0) * factor
    other = jnp.clip(jax.random.normal(other_part, shape, jnp.float32), -6.0, 6.0) * factor
    return (key_matrix, other)


def query_draw(key, index):
    key_matrix, other = pair_draw(key, index)
    return jnp.clip(2.0 * other, -6.0, 6.0).astype(jnp.bfloat16)


def draw_query_one(key, part):
    return query_draw(key, 11)


def draw_key_one(key, part):
    return pair_draw(key, 11)[0].astype(jnp.bfloat16)


def draw_query_two(key, part):
    return query_draw(key, 12)


def draw_key_two(key, part):
    return pair_draw(key, 12)[0].astype(jnp.bfloat16)


def block_levels(stream_key, extent, cuts, low, high):
    factor_of = 1.0
    for axis_at, blocks in cuts:
        steps = jax.random.uniform(jax.random.fold_in(jax.random.fold_in(stream_key, 6), axis_at), (blocks,), jnp.float32, low / len(cuts), high / len(cuts))
        factor_of = factor_of * jnp.repeat(jnp.exp(steps), extent[axis_at] // blocks).reshape((-1,) + (1,) * (len(extent) - 1 - axis_at))
    return factor_of


def gaussian(own_key, shape, scale, limit, pieces=(), kind=jnp.bfloat16):
    drawn = jax.random.normal(own_key, shape, jnp.float32) * scale
    if len(pieces) > 0:
        drawn = block_levels(own_key, shape, pieces, -0.22, 0.18) * drawn
    return jnp.clip(drawn, min=-limit, max=limit).astype(kind)


def setup_inputs(seed: int = 0) -> dict:
    seeds = jax.random.split(jax.random.key(seed), 17)
    return {
        "tokens": draw_tokens(jax.random.fold_in(seeds[16], 71), 0),
        "norm_gain": jnp.clip(1.0 + 0.18 * jax.random.normal(seeds[1], (D,), jnp.float32), 0.1, 1.9),
        "query_one": draw_query_one(jax.random.fold_in(seeds[16], 71), 0),
        "key_one": draw_key_one(jax.random.fold_in(seeds[16], 71), 0),
        "query_two": draw_query_two(jax.random.fold_in(seeds[16], 71), 0),
        "key_two": draw_key_two(jax.random.fold_in(seeds[16], 71), 0),
        "value_weight": gaussian(seeds[6], (D, HEADS * VALUE_DIM), D ** -0.5, 0.125, ((1, 2),)),
        "attn_gate_weight": gaussian(seeds[7], (D, HEADS * VALUE_DIM), D ** -0.5, 0.125, ((1, 2),)),
        "conv_outer": gaussian(seeds[8], (D, CONV_CH), D ** -0.5, 0.125, ((1, 2),)),
        "conv_inner": gaussian(seeds[9], (D, CONV_CH), D ** -0.5, 0.125, ((1, 2),)),
        "conv_input": gaussian(seeds[10], (D, CONV_CH), D ** -0.5, 0.125, ((1, 2),)),
        "conv_taps": gaussian(seeds[11], (3, CONV_CH), 3 ** -0.5, 3.5, ((1, 2),)),
        "head_lambda": jnp.clip(0.3 + 0.5 * jax.random.uniform(seeds[12], (HEADS,), jnp.float32) ** block_levels(seeds[12], (HEADS,), ((0, 2),), -0.2, 0.2), 0.3, 0.8),
        "head_gain": jnp.clip(1.0 + 0.18 * jax.random.normal(seeds[13], (VALUE_DIM,), jnp.float32), 0.1, 1.9),
        "attn_out_weight": gaussian(seeds[14], (HEADS * VALUE_DIM, D), (HEADS * VALUE_DIM + CONV_CH) ** -0.5, 0.125, ((0, 2),)),
        "conv_out_weight": gaussian(seeds[15], (CONV_CH, D), (HEADS * VALUE_DIM + CONV_CH) ** -0.5, 0.125, ((0, 2),)),
    }


EPSILON = 1e-06

def one_map(queries, keys, values):
    scores = jnp.dot(queries, keys.T, preferred_element_type=jnp.float32) * (1.0 / math.sqrt(KEY_DIM))
    peak = lax.optimization_barrier(jnp.max(scores, axis=1, keepdims=True))
    weights = jnp.exp(scores - peak)
    totals = lax.optimization_barrier(jnp.sum(weights, axis=1, keepdims=True))
    return jnp.dot(weights.astype(jnp.bfloat16), values, preferred_element_type=jnp.float32) / totals

def reference(tokens, norm_gain, query_one, key_one, query_two, key_two, value_weight, attn_gate_weight, conv_outer, conv_inner, conv_input, conv_taps, head_lambda, head_gain, attn_out_weight, conv_out_weight):
    wide = tokens.astype(jnp.float32)
    inv_rms = lax.rsqrt(lax.optimization_barrier(jnp.mean(wide * wide, axis=1, keepdims=True)) + EPSILON)
    scaled = (wide * norm_gain.astype(jnp.float32)).astype(jnp.bfloat16)

    def project(matrix):
        return (jnp.dot(scaled, matrix, preferred_element_type=jnp.float32) * inv_rms).astype(jnp.bfloat16)
    first_query = project(query_one)
    first_key = project(key_one)
    second_query = project(query_two)
    second_key = project(key_two)
    values = project(value_weight)
    attn_gate = project(attn_gate_weight)
    outer = project(conv_outer)
    inner_a = project(conv_inner)
    inner_b = project(conv_input)
    block = math.gcd(TOKENS, 512)
    gain_head = head_gain.astype(jnp.float32)

    def by_head(matrix, width):
        return matrix.reshape(TOKENS, HEADS, width).transpose(1, 0, 2)

    def per_head(head_args):
        query_a, key_a, query_b, key_b, head_values, head_gate, weight_b = head_args

        def per_block(block_args):
            block_a, block_b, block_gate = block_args
            diff = one_map(block_a, key_a, head_values) - weight_b * one_map(block_b, key_b, head_values)
            normed = diff * lax.rsqrt(lax.optimization_barrier(jnp.mean(diff * diff, axis=1, keepdims=True)) + EPSILON) * gain_head
            return (normed * jax.nn.silu(block_gate.astype(jnp.float32))).astype(jnp.bfloat16)
        outputs = lax.map(per_block, (query_a.reshape(-1, block, KEY_DIM), query_b.reshape(-1, block, KEY_DIM), head_gate.reshape(-1, block, VALUE_DIM)))
        return outputs.reshape(TOKENS, VALUE_DIM)
    heads_out = lax.map(per_head, (by_head(first_query, KEY_DIM), by_head(first_key, KEY_DIM), by_head(second_query, KEY_DIM), by_head(second_key, KEY_DIM), by_head(values, VALUE_DIM), by_head(attn_gate, VALUE_DIM), head_lambda.astype(jnp.float32)))
    attn_mix = heads_out.transpose(1, 0, 2).reshape(TOKENS, HEADS * VALUE_DIM)
    product = (inner_a.astype(jnp.float32) * inner_b.astype(jnp.float32)).astype(jnp.bfloat16)
    padded = jnp.pad(product.astype(jnp.float32), ((1, 1), (0, 0)))
    taps = conv_taps.astype(jnp.float32)
    convolved = taps[0] * padded[:-2] + taps[1] * padded[1:-1] + taps[2] * padded[2:]
    conv_mix = (outer.astype(jnp.float32) * convolved).astype(jnp.bfloat16)
    head_width = HEADS // N_TP * VALUE_DIM
    conv_width = CONV_CH // N_TP
    mixed = jnp.zeros((TOKENS, D), jnp.float32)
    for group in range(N_TP):
        partial_sum = jnp.dot(attn_mix[:, group * head_width:(group + 1) * head_width], attn_out_weight[group * head_width:(group + 1) * head_width], preferred_element_type=jnp.float32)
        partial_sum = partial_sum + jnp.dot(conv_mix[:, group * conv_width:(group + 1) * conv_width], conv_out_weight[group * conv_width:(group + 1) * conv_width], preferred_element_type=jnp.float32)
        rounded = lax.optimization_barrier(partial_sum.astype(jnp.bfloat16))
        mixed = mixed + rounded.astype(jnp.float32)
    return mixed.astype(jnp.bfloat16)
```

```python
import functools
import math

import jax
import jax.numpy as jnp
from jax import lax
from jax.experimental import pallas as pl
from jax.experimental.pallas import tpu as pltpu
from jax.sharding import PartitionSpec as P

EPSILON = 1e-06
MESH = pl.DeviceIdType.MESH
F32 = jnp.float32
BF16 = jnp.bfloat16
HALO = 16


def remote(src, dst, send_sem, recv_sem, sp, tp):
    return pltpu.make_async_remote_copy(
        src_ref=src,
        dst_ref=dst,
        send_sem=send_sem,
        recv_sem=recv_sem,
        device_id=(sp, tp),
        device_id_type=MESH,
    )


def kernel(
    S,
    T,
    H,
    KD,
    VD,
    tokens,
    gain,
    taps,
    head_gain,
    lam,
    w_k1,
    w_k2,
    w_v,
    w_q1,
    w_q2,
    w_ia,
    w_ib,
    w_outer,
    w_gate,
    w_ao,
    w_co,
    out,
    s_k1,
    s_k2,
    s_v,
    s_q1,
    s_q2,
    s_ia,
    s_ib,
    s_outer,
    s_gate,
    s_ao,
    s_co,
    tok,
    scaled,
    kv_send,
    kv_all,
    q_send,
    q_all,
    qz,
    acc,
    peak,
    total,
    prod,
    halo_lo,
    halo_hi,
    outer_y,
    gate_y,
    pre,
    att_out,
    att_in,
    mix,
    part_send,
    part_in,
    w_sem,
    tok_ss,
    tok_rs,
    kv_ss,
    kv_rs,
    fw_ss,
    q_ss,
    q_rs,
    halo_ss,
    halo_rs,
    att_ss,
    att_rs,
    part_ss,
    part_rs,
):
    G = S // H
    R, DT = tokens.shape
    D = DT * T
    me = lax.axis_index("sp")
    t = lax.axis_index("tp")
    h = me // G
    c = me % G

    hbm = (w_k1, w_k2, w_v, w_q1, w_q2, w_ia, w_ib, w_outer, w_gate, w_co, w_ao)
    vmem = (s_k1, s_k2, s_v, s_q1, s_q2, s_ia, s_ib, s_outer, s_gate, s_co, s_ao)
    loads = [pltpu.make_async_copy(a, b, w_sem.at[i]) for i, (a, b) in enumerate(zip(hbm, vmem))]
    for load in loads:
        load.start()
    ready = dict(zip([id(b) for b in vmem], loads))

    def tp_peer(k):
        return lax.rem(t + k, T)

    def head_peer(k):
        return lax.rem(h + k, H)

    def lane_peer(k):
        return lax.rem(c + k, G)

    lo = lax.rem(me + S - 1, S)
    hi = lax.rem(me + 1, S)

    barrier = pltpu.get_barrier_semaphore()
    greeted = 0
    for k in range(1, T):
        pl.semaphore_signal(barrier, inc=1, device_id=(me, tp_peer(k)), device_id_type=MESH)
        greeted += 1
    for k in range(1, H):
        pl.semaphore_signal(barrier, inc=1, device_id=(head_peer(k) * G + c, t), device_id_type=MESH)
        greeted += 1
    for k in range(1, G):
        pl.semaphore_signal(barrier, inc=1, device_id=(h * G + lane_peer(k), t), device_id_type=MESH)
        greeted += 1
    for other in (lo, hi):
        pl.semaphore_signal(barrier, inc=1, device_id=(other, t), device_id_type=MESH)
        greeted += 1
    pl.semaphore_wait(barrier, greeted)

    tok_copies = [
        remote(tokens, tok.at[t], tok_ss.at[k], tok_rs.at[k], me, tp_peer(k)) for k in range(1, T)
    ]
    for copy in tok_copies:
        copy.start()
    tok[t] = tokens[...]
    acc[...] = jnp.zeros_like(acc)
    peak[...] = jnp.full_like(peak, -1e30)
    total[...] = jnp.zeros_like(total)
    for copy in tok_copies:
        copy.wait()
    squares = jnp.zeros((R, 1), F32)
    for i in range(T):
        wide = tok[i].astype(F32)
        squares = squares + jnp.sum(wide * wide, axis=1, keepdims=True)
        scaled[:, i * DT : (i + 1) * DT] = (wide * gain[:, i * DT : (i + 1) * DT]).astype(BF16)
    inv = lax.rsqrt(squares / D + EPSILON)

    def project(w):
        ready[id(w)].wait()
        return jnp.dot(scaled[...], w[...], preferred_element_type=F32) * inv

    def halves(a, b, p):
        return jnp.concatenate(
            [a[:, p * KD : (p + 1) * KD], b[:, p * KD : (p + 1) * KD]], axis=1
        ).astype(BF16)

    k1 = project(s_k1)
    k2 = project(s_k2)
    for p in range(H):
        kv_send[p, :, : 2 * KD] = halves(k1, k2, p)
    values = project(s_v).astype(BF16)
    for p in range(H):
        kv_send[p, :, 2 * KD :] = values[:, p * VD : (p + 1) * VD]
    my_rows = pl.ds(pl.multiple_of(me * R, R), R)
    kv_copies = [
        remote(
            kv_send.at[head_peer(k)],
            kv_all.at[my_rows],
            kv_ss.at[k],
            kv_rs.at[me],
            head_peer(k) * G + c,
            t,
        )
        for k in range(1, H)
    ]
    for copy in kv_copies:
        copy.start()
    kv_all[my_rows] = kv_send[h]

    def arrival(source):
        rows = kv_all.at[pl.ds(pl.multiple_of(source * R, R), R)]
        return remote(rows, rows, fw_ss.at[0, 0], kv_rs.at[source], me, t)

    def forward(k, m):
        source = lax.rem(h + H - k, H) * G + c
        rows = kv_all.at[pl.ds(pl.multiple_of(source * R, R), R)]
        return remote(rows, rows, fw_ss.at[k, m], kv_rs.at[source], h * G + lane_peer(m), t)

    def forward_all(k):
        if k:
            arrival(lax.rem(h + H - k, H) * G + c).wait_recv()
        for m in range(1, G):
            forward(k, m).start()

    forward_all(0)

    q1 = project(s_q1)
    q2 = project(s_q2)
    for p in range(H):
        q_send[p] = halves(q1, q2, p)
    q_copies = [
        remote(
            q_send.at[head_peer(k)], q_all.at[h], q_ss.at[k], q_rs.at[h], head_peer(k) * G + c, t
        )
        for k in range(1, H)
    ]
    for copy in q_copies:
        copy.start()
    q_all[h] = q_send[h]

    inner_a = project(s_ia).astype(BF16).astype(F32)
    inner_b = project(s_ib).astype(BF16).astype(F32)
    prod[...] = (inner_a * inner_b).astype(BF16)
    halo_copies = [
        remote(prod.at[pl.ds(R - HALO, HALO)], halo_lo, halo_ss.at[0], halo_rs.at[0], hi, t),
        remote(prod.at[pl.ds(0, HALO)], halo_hi, halo_ss.at[1], halo_rs.at[1], lo, t),
    ]
    for copy in halo_copies:
        copy.start()
    if H > 1:
        forward_all(1)
    outer_y[...] = project(s_outer).astype(BF16)
    if H > 2:
        forward_all(2)
    gate_y[...] = project(s_gate).astype(BF16)
    for k in range(3, H):
        forward_all(k)

    for copy in halo_copies:
        copy.wait()
    wide = prod[...].astype(F32)
    row = lax.broadcasted_iota(jnp.int32, wide.shape, 0)
    first = jnp.where(me == 0, 0.0, halo_lo[...].astype(F32)[HALO - 1 : HALO])
    last = jnp.where(me == S - 1, 0.0, halo_hi[...].astype(F32)[0:1])
    before = jnp.where(row == 0, first, pltpu.roll(wide, 1, 0))
    after = jnp.where(row == R - 1, last, pltpu.roll(wide, R - 1, 0))
    tap = taps[...].astype(F32)
    convolved = tap[0:1] * before + tap[1:2] * wide + tap[2:3] * after
    conv_mix = (outer_y[...].astype(F32) * convolved).astype(BF16)
    ready[id(s_co)].wait()
    pre[...] = jnp.dot(conv_mix, s_co[...], preferred_element_type=F32)

    for k in range(1, H):
        source = lax.rem(h + H - k, H)
        remote(q_all.at[source], q_all.at[source], q_ss.at[k], q_rs.at[source], me, t).wait_recv()
    for p in range(H):
        both = q_all[p].astype(F32)
        lane = lax.broadcasted_iota(jnp.int32, both.shape, 1)
        qz[p, :R] = jnp.where(lane < KD, both, 0.0).astype(BF16)
        qz[p, R:] = jnp.where(lane < KD, 0.0, both).astype(BF16)

    group = G * R
    block = math.gcd(group, 1024)
    chunks = group // block
    factor = math.log2(math.e) / math.sqrt(KD)
    my_lam = lam[h]

    def finish(j, qi):
        state = acc[qi] / total[qi]
        diff = state[:R] - my_lam * state[R:]
        normed = diff * lax.rsqrt(jnp.mean(diff * diff, axis=1, keepdims=True) + EPSILON)
        att_out[qi] = (normed * head_gain[...]).astype(BF16)

        if H > 1:

            @pl.when(j < H - 1)
            def _():
                remote(
                    att_out.at[qi], att_in.at[h], att_ss.at[j], att_rs.at[h], qi * G + c, t
                ).start()

        @pl.when(j == H - 1)
        def _():
            att_in[h] = att_out[qi]

    def one_group(k, carry):
        source_head = lax.rem(h + H - k, H)
        for m in range(1, G):
            arrival(source_head * G + lane_peer(m)).wait_recv()

        def one_chunk(step, inner):
            ch = step // H
            j = lax.rem(step, H)
            qi = lax.rem(h + 1 + j, H)
            keys = pl.ds(pl.multiple_of(source_head * group + ch * block, block), block)
            scores = lax.dot_general(
                qz[qi],
                kv_all[keys, : 2 * KD],
                (((1,), (1,)), ((), ())),
                preferred_element_type=F32,
            )
            old = peak[qi]
            new = jnp.maximum(old, jnp.max(scores, axis=1, keepdims=True))
            weights = jnp.exp2((scores - new) * factor)
            scale = jnp.exp2((old - new) * factor)
            total[qi] = total[qi] * scale + jnp.sum(weights, axis=1, keepdims=True)
            acc[qi] = acc[qi] * scale + jnp.dot(
                weights.astype(BF16), kv_all[keys, 2 * KD :], preferred_element_type=F32
            )
            peak[qi] = new

            @pl.when((k == H - 1) & (ch == chunks - 1))
            def _():
                finish(j, qi)

            return inner

        lax.fori_loop(0, chunks * H, one_chunk, 0)
        return carry

    lax.fori_loop(0, H, one_group, 0)

    for k in range(1, H):
        source = lax.rem(h + H - k, H)
        remote(
            att_in.at[source], att_in.at[source], att_ss.at[0], att_rs.at[source], me, t
        ).wait_recv()
    for p in range(H):
        gate = gate_y[:, p * VD : (p + 1) * VD].astype(F32)
        mix[:, p * VD : (p + 1) * VD] = (
            att_in[p].astype(F32) * (gate / (1.0 + jnp.exp(-gate)))
        ).astype(BF16)
    ready[id(s_ao)].wait()
    RT = R // T

    def partial(owner):
        rows = pl.ds(pl.multiple_of(owner * RT, RT), RT)
        return (
            jnp.dot(mix[rows], s_ao[...], preferred_element_type=F32) + pre[rows]
        ).astype(BF16)

    part_copies = []
    for k in range(1, T):
        part_send[k - 1] = partial(tp_peer(k))
        copy = remote(
            part_send.at[k - 1], part_in.at[k - 1], part_ss.at[k], part_rs.at[k], me, tp_peer(k)
        )
        copy.start()
        part_copies.append(copy)
    mixed = partial(t).astype(F32)
    for k, copy in enumerate(part_copies):
        copy.wait()
        mixed = mixed + part_in[k].astype(F32)
    out[...] = mixed.astype(BF16)

    for copy in kv_copies + q_copies:
        copy.wait_send()
    for k in range(H):
        for m in range(1, G):
            forward(k, m).wait_send()
    for j in range(H - 1):
        qi = lax.rem(h + 1 + j, H)
        remote(att_out.at[qi], att_in.at[h], att_ss.at[j], att_rs.at[h], qi * G + c, t).wait_send()


def local(
    S,
    T,
    tokens,
    norm_gain,
    query_one,
    key_one,
    query_two,
    key_two,
    value_weight,
    attn_gate_weight,
    conv_outer,
    conv_inner,
    conv_input,
    conv_taps,
    head_lambda,
    head_gain,
    attn_out_weight,
    conv_out_weight,
):
    R, DT = tokens.shape
    D = DT * T
    H = head_lambda.shape[0]
    KD = key_one.shape[1] // H
    VD = value_weight.shape[1] // H
    C = conv_taps.shape[1]
    G = S // H
    RT = R // T
    weights = (
        key_one,
        key_two,
        value_weight,
        query_one,
        query_two,
        conv_inner,
        conv_input,
        conv_outer,
        attn_gate_weight,
        attn_out_weight,
        conv_out_weight,
    )
    vm = pl.BlockSpec(memory_space=pltpu.VMEM)
    dma = pltpu.SemaphoreType.DMA
    return pl.pallas_call(
        functools.partial(kernel, S, T, H, KD, VD),
        out_shape=jax.ShapeDtypeStruct((RT, D), BF16),
        in_specs=[vm] * 4
        + [pl.BlockSpec(memory_space=pltpu.SMEM)]
        + [pl.BlockSpec(memory_space=pl.ANY)] * len(weights),
        out_specs=vm,
        scratch_shapes=[pltpu.VMEM(w.shape, BF16) for w in weights]
        + [
            pltpu.VMEM((T, R, DT), BF16),
            pltpu.VMEM((R, D), BF16),
            pltpu.VMEM((H, R, 2 * KD + VD), BF16),
            pltpu.VMEM((S * R, 2 * KD + VD), BF16),
            pltpu.VMEM((H, R, 2 * KD), BF16),
            pltpu.VMEM((H, R, 2 * KD), BF16),
            pltpu.VMEM((H, 2 * R, 2 * KD), BF16),
            pltpu.VMEM((H, 2 * R, VD), F32),
            pltpu.VMEM((H, 2 * R, 1), F32),
            pltpu.VMEM((H, 2 * R, 1), F32),
            pltpu.VMEM((R, C), BF16),
            pltpu.VMEM((HALO, C), BF16),
            pltpu.VMEM((HALO, C), BF16),
            pltpu.VMEM((R, C), BF16),
            pltpu.VMEM((R, H * VD), BF16),
            pltpu.VMEM((R, D), F32),
            pltpu.VMEM((H, R, VD), BF16),
            pltpu.VMEM((H, R, VD), BF16),
            pltpu.VMEM((R, H * VD), BF16),
            pltpu.VMEM((max(T - 1, 1), RT, D), BF16),
            pltpu.VMEM((max(T - 1, 1), RT, D), BF16),
            dma((len(weights),)),
            dma((T,)),
            dma((T,)),
            dma((H,)),
            dma((S,)),
            dma((H, G)),
            dma((H,)),
            dma((H,)),
            dma((2,)),
            dma((2,)),
            dma((H,)),
            dma((H,)),
            dma((T,)),
            dma((T,)),
        ],
        compiler_params=pltpu.CompilerParams(
            collective_id=0, has_side_effects=True, vmem_limit_bytes=60 * 1024 * 1024
        ),
        name="layer",
    )(
        tokens,
        norm_gain.reshape(1, D),
        conv_taps,
        head_gain.reshape(1, VD),
        head_lambda,
        *weights,
    )


def solution(mesh):
    S = mesh.shape["sp"]
    T = mesh.shape["tp"]
    return jax.shard_map(
        functools.partial(local, S, T),
        mesh=mesh,
        in_specs=(P("sp", "tp"), P())
        + (P(None, "tp"),) * 10
        + (P("tp"), P(), P("tp", None), P("tp", None)),
        out_specs=P(("sp", "tp"), None),
        check_vma=False,
    )
```

```python
import functools
import math

import jax
import jax.numpy as jnp
from jax import lax
from jax.experimental import pallas as pl
from jax.experimental.pallas import tpu as pltpu
from jax.sharding import PartitionSpec as P

EPSILON = 1e-06
MESH = pl.DeviceIdType.MESH
F32 = jnp.float32
BF16 = jnp.bfloat16
HALO = 16
TILES = 4


def remote(src, dst, send_sem, recv_sem, sp, tp):
    return pltpu.make_async_remote_copy(
        src_ref=src,
        dst_ref=dst,
        send_sem=send_sem,
        recv_sem=recv_sem,
        device_id=(sp, tp),
        device_id_type=MESH,
    )


def kernel(
    S,
    T,
    H,
    KD,
    VD,
    tokens,
    gain,
    taps,
    head_gain,
    lam,
    w_k1,
    w_k2,
    w_v,
    w_q1,
    w_q2,
    w_ia,
    w_ib,
    w_outer,
    w_gate,
    w_ao,
    w_co,
    out,
    s_k1,
    s_k2,
    s_v,
    s_q1,
    s_q2,
    s_ia,
    s_ib,
    s_outer,
    s_gate,
    s_ao,
    s_co,
    tok,
    scaled,
    kv_send,
    kv_all,
    q_send,
    q_all,
    qz,
    acc,
    peak,
    total,
    prod,
    halo_lo,
    halo_hi,
    outer_y,
    gate_y,
    pre,
    att_out,
    att_in,
    mix,
    part_send,
    part_in,
    w_sem,
    tok_ss,
    tok_rs,
    kv_ss,
    kv_rs,
    fw_ss,
    q_ss,
    q_rs,
    halo_ss,
    halo_rs,
    att_ss,
    att_rs,
    part_ss,
    part_rs,
):
    G = S // H
    R, DT = tokens.shape
    D = DT * T
    me = lax.axis_index("sp")
    t = lax.axis_index("tp")
    h = me // G
    c = me % G

    hbm = (w_k1, w_k2, w_v, w_q1, w_q2, w_ia, w_ib, w_outer, w_gate, w_co, w_ao)
    vmem = (s_k1, s_k2, s_v, s_q1, s_q2, s_ia, s_ib, s_outer, s_gate, s_co, s_ao)
    loads = [pltpu.make_async_copy(a, b, w_sem.at[i]) for i, (a, b) in enumerate(zip(hbm, vmem))]
    for load in loads:
        load.start()
    ready = dict(zip([id(b) for b in vmem], loads))

    def tp_peer(k):
        return lax.rem(t + k, T)

    def head_peer(k):
        return lax.rem(h + k, H)

    def lane_peer(k):
        return lax.rem(c + k, G)

    lo = lax.rem(me + S - 1, S)
    hi = lax.rem(me + 1, S)

    barrier = pltpu.get_barrier_semaphore()
    greeted = 0
    for k in range(1, T):
        pl.semaphore_signal(barrier, inc=1, device_id=(me, tp_peer(k)), device_id_type=MESH)
        greeted += 1
    for k in range(1, H):
        pl.semaphore_signal(barrier, inc=1, device_id=(head_peer(k) * G + c, t), device_id_type=MESH)
        greeted += 1
    for k in range(1, G):
        pl.semaphore_signal(barrier, inc=1, device_id=(h * G + lane_peer(k), t), device_id_type=MESH)
        greeted += 1
    for other in (lo, hi):
        pl.semaphore_signal(barrier, inc=1, device_id=(other, t), device_id_type=MESH)
        greeted += 1
    pl.semaphore_wait(barrier, greeted)

    tok_copies = [
        remote(tokens, tok.at[t], tok_ss.at[k], tok_rs.at[k], me, tp_peer(k)) for k in range(1, T)
    ]
    for copy in tok_copies:
        copy.start()
    tok[t] = tokens[...]
    acc[...] = jnp.zeros_like(acc)
    peak[...] = jnp.full_like(peak, -1e30)
    total[...] = jnp.zeros_like(total)
    for copy in tok_copies:
        copy.wait()
    squares = jnp.zeros((R, 1), F32)
    for i in range(T):
        wide = tok[i].astype(F32)
        squares = squares + jnp.sum(wide * wide, axis=1, keepdims=True)
        scaled[:, i * DT : (i + 1) * DT] = (wide * gain[:, i * DT : (i + 1) * DT]).astype(BF16)
    inv = lax.rsqrt(squares / D + EPSILON)

    def project(w):
        ready[id(w)].wait()
        return jnp.dot(scaled[...], w[...], preferred_element_type=F32) * inv

    def halves(a, b, p):
        return jnp.concatenate(
            [a[:, p * KD : (p + 1) * KD], b[:, p * KD : (p + 1) * KD]], axis=1
        ).astype(BF16)

    k1 = project(s_k1)
    k2 = project(s_k2)
    for p in range(H):
        kv_send[p, :, : 2 * KD] = halves(k1, k2, p)
    values = project(s_v).astype(BF16)
    for p in range(H):
        kv_send[p, :, 2 * KD :] = values[:, p * VD : (p + 1) * VD]
    my_rows = pl.ds(pl.multiple_of(me * R, R), R)
    kv_copies = [
        remote(
            kv_send.at[head_peer(k)],
            kv_all.at[my_rows],
            kv_ss.at[k],
            kv_rs.at[me],
            head_peer(k) * G + c,
            t,
        )
        for k in range(1, H)
    ]
    for copy in kv_copies:
        copy.start()
    kv_all[my_rows] = kv_send[h]

    def arrival(source):
        rows = kv_all.at[pl.ds(pl.multiple_of(source * R, R), R)]
        return remote(rows, rows, fw_ss.at[0, 0], kv_rs.at[source], me, t)

    def forward(k, m):
        source = lax.rem(h + H - k, H) * G + c
        rows = kv_all.at[pl.ds(pl.multiple_of(source * R, R), R)]
        return remote(rows, rows, fw_ss.at[k, m], kv_rs.at[source], h * G + lane_peer(m), t)

    def forward_all(k):
        if not (isinstance(k, int) and k == 0):
            arrival(lax.rem(h + H - k, H) * G + c).wait_recv()
        for m in range(1, G):
            forward(k, m).start()

    forward_all(0)

    q1 = project(s_q1)
    q2 = project(s_q2)
    for p in range(H):
        q_send[p] = halves(q1, q2, p)
    q_copies = [
        remote(
            q_send.at[head_peer(k)], q_all.at[h], q_ss.at[k], q_rs.at[h], head_peer(k) * G + c, t
        )
        for k in range(1, H)
    ]
    for copy in q_copies:
        copy.start()
    q_all[h] = q_send[h]

    inner_a = project(s_ia).astype(BF16).astype(F32)
    inner_b = project(s_ib).astype(BF16).astype(F32)
    prod[...] = (inner_a * inner_b).astype(BF16)
    halo_copies = [
        remote(prod.at[pl.ds(R - HALO, HALO)], halo_lo, halo_ss.at[0], halo_rs.at[0], hi, t),
        remote(prod.at[pl.ds(0, HALO)], halo_hi, halo_ss.at[1], halo_rs.at[1], lo, t),
    ]
    for copy in halo_copies:
        copy.start()
    if H > 1:
        forward_all(1)
    outer_y[...] = project(s_outer).astype(BF16)
    if H > 2:
        forward_all(2)
    gate_y[...] = project(s_gate).astype(BF16)

    for k in range(3, H):
        forward_all(k)

    for copy in halo_copies:
        copy.wait()
    wide = prod[...].astype(F32)
    row = lax.broadcasted_iota(jnp.int32, wide.shape, 0)
    first = jnp.where(me == 0, 0.0, halo_lo[...].astype(F32)[HALO - 1 : HALO])
    last = jnp.where(me == S - 1, 0.0, halo_hi[...].astype(F32)[0:1])
    before = jnp.where(row == 0, first, pltpu.roll(wide, 1, 0))
    after = jnp.where(row == R - 1, last, pltpu.roll(wide, R - 1, 0))
    tap = taps[...].astype(F32)
    convolved = tap[0:1] * before + tap[1:2] * wide + tap[2:3] * after
    conv_mix = (outer_y[...].astype(F32) * convolved).astype(BF16)
    ready[id(s_co)].wait()
    pre[...] = jnp.dot(conv_mix, s_co[...], preferred_element_type=F32)

    for k in range(1, H):
        source = lax.rem(h + H - k, H)
        remote(q_all.at[source], q_all.at[source], q_ss.at[k], q_rs.at[source], me, t).wait_recv()
    for p in range(H):
        both = q_all[p].astype(F32)
        lane = lax.broadcasted_iota(jnp.int32, both.shape, 1)
        qz[p, :R] = jnp.where(lane < KD, both, 0.0).astype(BF16)
        qz[p, R:] = jnp.where(lane < KD, 0.0, both).astype(BF16)

    group = G * R
    block = math.gcd(group, 1024)
    chunks = group // block
    factor = math.log2(math.e) / math.sqrt(KD)
    my_lam = lam[h]

    def finish(j, qi):
        state = acc[qi] / total[qi]
        diff = state[:R] - my_lam * state[R:]
        normed = diff * lax.rsqrt(jnp.mean(diff * diff, axis=1, keepdims=True) + EPSILON)
        att_out[qi] = (normed * head_gain[...]).astype(BF16)

        if H > 1:

            @pl.when(j < H - 1)
            def _():
                remote(
                    att_out.at[qi], att_in.at[h], att_ss.at[j], att_rs.at[h], qi * G + c, t
                ).start()

        @pl.when(j == H - 1)
        def _():
            att_in[h] = att_out[qi]

    def one_group(k, carry):
        source_head = lax.rem(h + H - k, H)
        for m in range(1, G):
            arrival(source_head * G + lane_peer(m)).wait_recv()

        def one_chunk(step, inner):
            ch = step // H
            j = lax.rem(step, H)
            qi = lax.rem(h + 1 + j, H)
            keys = pl.ds(pl.multiple_of(source_head * group + ch * block, block), block)
            keys_ref = kv_all[keys, : 2 * KD]
            vals_ref = kv_all[keys, 2 * KD :]
            tile = 2 * R // TILES

            def score(i):
                return lax.dot_general(
                    qz[qi, i * tile : (i + 1) * tile],
                    keys_ref,
                    (((1,), (1,)), ((), ())),
                    preferred_element_type=F32,
                )

            def soften(i, scores):
                rows = slice(i * tile, (i + 1) * tile)
                old = peak[qi, rows]
                new = jnp.maximum(old, jnp.max(scores, axis=1, keepdims=True))
                spread = jnp.concatenate([new] * (block // new.shape[1]), axis=1)
                weights = jnp.exp2((scores - spread) * factor)
                scale = jnp.exp2((old - new) * factor)
                total[qi, rows] = total[qi, rows] * scale + jnp.sum(weights, axis=1, keepdims=True)
                peak[qi, rows] = new
                return weights.astype(BF16), scale

            def gather(i, weights, scale):
                rows = slice(i * tile, (i + 1) * tile)
                acc[qi, rows] = acc[qi, rows] * scale + jnp.dot(
                    weights, vals_ref, preferred_element_type=F32
                )

            ahead = score(0)
            held = None
            for i in range(TILES):
                current = ahead
                if i + 1 < TILES:
                    ahead = score(i + 1)
                if held is not None:
                    gather(i - 1, *held)
                held = soften(i, current)
            gather(TILES - 1, *held)

            @pl.when((k == H - 1) & (ch == chunks - 1))
            def _():
                finish(j, qi)

            return inner

        lax.fori_loop(0, chunks * H, one_chunk, 0)
        return carry

    lax.fori_loop(0, H, one_group, 0)

    for k in range(1, H):
        source = lax.rem(h + H - k, H)
        remote(
            att_in.at[source], att_in.at[source], att_ss.at[0], att_rs.at[source], me, t
        ).wait_recv()
    for p in range(H):
        gate = gate_y[:, p * VD : (p + 1) * VD].astype(F32)
        mix[:, p * VD : (p + 1) * VD] = (
            att_in[p].astype(F32) * (gate / (1.0 + jnp.exp(-gate)))
        ).astype(BF16)
    ready[id(s_ao)].wait()
    RT = R // T

    def partial(owner):
        rows = pl.ds(pl.multiple_of(owner * RT, RT), RT)
        return (
            jnp.dot(mix[rows], s_ao[...], preferred_element_type=F32) + pre[rows]
        ).astype(BF16)

    part_copies = []
    for k in range(1, T):
        part_send[k - 1] = partial(tp_peer(k))
        copy = remote(
            part_send.at[k - 1], part_in.at[k - 1], part_ss.at[k], part_rs.at[k], me, tp_peer(k)
        )
        copy.start()
        part_copies.append(copy)
    mixed = partial(t).astype(F32)
    for k, copy in enumerate(part_copies):
        copy.wait()
        mixed = mixed + part_in[k].astype(F32)
    out[...] = mixed.astype(BF16)

    for copy in kv_copies + q_copies:
        copy.wait_send()
    for k in range(H):
        for m in range(1, G):
            forward(k, m).wait_send()
    for j in range(H - 1):
        qi = lax.rem(h + 1 + j, H)
        remote(att_out.at[qi], att_in.at[h], att_ss.at[j], att_rs.at[h], qi * G + c, t).wait_send()


def local(
    S,
    T,
    tokens,
    norm_gain,
    query_one,
    key_one,
    query_two,
    key_two,
    value_weight,
    attn_gate_weight,
    conv_outer,
    conv_inner,
    conv_input,
    conv_taps,
    head_lambda,
    head_gain,
    attn_out_weight,
    conv_out_weight,
):
    R, DT = tokens.shape
    D = DT * T
    H = head_lambda.shape[0]
    KD = key_one.shape[1] // H
    VD = value_weight.shape[1] // H
    C = conv_taps.shape[1]
    G = S // H
    RT = R // T
    weights = (
        key_one,
        key_two,
        value_weight,
        query_one,
        query_two,
        conv_inner,
        conv_input,
        conv_outer,
        attn_gate_weight,
        attn_out_weight,
        conv_out_weight,
    )
    vm = pl.BlockSpec(memory_space=pltpu.VMEM)
    dma = pltpu.SemaphoreType.DMA
    return pl.pallas_call(
        functools.partial(kernel, S, T, H, KD, VD),
        out_shape=jax.ShapeDtypeStruct((RT, D), BF16),
        in_specs=[vm] * 4
        + [pl.BlockSpec(memory_space=pltpu.SMEM)]
        + [pl.BlockSpec(memory_space=pl.ANY)] * len(weights),
        out_specs=vm,
        scratch_shapes=[pltpu.VMEM(w.shape, BF16) for w in weights]
        + [
            pltpu.VMEM((T, R, DT), BF16),
            pltpu.VMEM((R, D), BF16),
            pltpu.VMEM((H, R, 2 * KD + VD), BF16),
            pltpu.VMEM((S * R, 2 * KD + VD), BF16),
            pltpu.VMEM((H, R, 2 * KD), BF16),
            pltpu.VMEM((H, R, 2 * KD), BF16),
            pltpu.VMEM((H, 2 * R, 2 * KD), BF16),
            pltpu.VMEM((H, 2 * R, VD), F32),
            pltpu.VMEM((H, 2 * R, VD), F32),
            pltpu.VMEM((H, 2 * R, VD), F32),
            pltpu.VMEM((R, C), BF16),
            pltpu.VMEM((HALO, C), BF16),
            pltpu.VMEM((HALO, C), BF16),
            pltpu.VMEM((R, C), BF16),
            pltpu.VMEM((R, H * VD), BF16),
            pltpu.VMEM((R, D), F32),
            pltpu.VMEM((H, R, VD), BF16),
            pltpu.VMEM((H, R, VD), BF16),
            pltpu.VMEM((R, H * VD), BF16),
            pltpu.VMEM((max(T - 1, 1), RT, D), BF16),
            pltpu.VMEM((max(T - 1, 1), RT, D), BF16),
            dma((len(weights),)),
            dma((T,)),
            dma((T,)),
            dma((H,)),
            dma((S,)),
            dma((H, G)),
            dma((H,)),
            dma((H,)),
            dma((2,)),
            dma((2,)),
            dma((H,)),
            dma((H,)),
            dma((T,)),
            dma((T,)),
        ],
        compiler_params=pltpu.CompilerParams(
            collective_id=0, has_side_effects=True, vmem_limit_bytes=60 * 1024 * 1024
        ),
        name="layer",
    )(
        tokens,
        norm_gain.reshape(1, D),
        conv_taps,
        head_gain.reshape(1, VD),
        head_lambda,
        *weights,
    )


def solution(mesh):
    S = mesh.shape["sp"]
    T = mesh.shape["tp"]
    return jax.shard_map(
        functools.partial(local, S, T),
        mesh=mesh,
        in_specs=(P("sp", "tp"), P())
        + (P(None, "tp"),) * 10
        + (P("tp"), P(), P("tp", None), P("tp", None)),
        out_specs=P(("sp", "tp"), None),
        check_vma=False,
    )
```
